128 devices in a mesh: fs: 16 (over z, y), tp: 8 (over x, core).
Axes of the slice: x: 4, y: 4, z: 4, core: 2. Of those that a mesh axis runs over, the one named last changes fastest.
Arguments:
- tokens: bfloat16 [32768, 2048], P('fs'), may hold values from -6 to 6
- norm_gain: float32 [2048], replicated, may hold values from 0.1 to 1.9
- gate_weight: bfloat16 [2048, 5632], P('fs', 'tp'), may hold values from -0.125 to 0.125
- up_weight: bfloat16 [2048, 5632], P('fs', 'tp'), may hold values from -0.125 to 0.125
- down_weight: bfloat16 [5632, 2048], P('tp', 'fs'), may hold values from -0.078125 to 0.078125
Outputs:
- mixed: bfloat16 [32768, 2048], P(('fs', 'tp'))
The draws below stay inside these ranges and needn't reach their ends.
All inputs are finite; a program needn't handle non-finite values.
Results may differ from the reference program's by a relative error of at most 0.014.
Values may be sent and summed in bfloat16 or wider, within the bound.
No kernel may reach another device: no remote copies, remote signals or barrier semaphores. Data moves between devices by JAX's collectives and lax.ppermute only.
A program may use at most 128 MiB of HBM per device.

```python
import jax
import jax.numpy as jnp
from jax import lax

D = 2048
FF = 5632
TOKENS = 32768
N_FS = 16
N_TP = 8


def block_scale(own_key, extent, cuts, low, high):
    loudness = 1.0
    for axis_at, blocks in cuts:
        heights = jax.random.uniform(jax.random.fold_in(jax.random.fold_in(own_key, 6), axis_at), (blocks,), jnp.float32, low / len(cuts), high / len(cuts))
        loudness = loudness * jnp.repeat(jnp.exp(heights), extent[axis_at] // blocks).reshape((-1,) + (1,) * (len(extent) - 1 - axis_at))
    return loudness


def gaussian(key, dims, spread, limit, shards=(), kind=jnp.bfloat16):
    values = jax.random.normal(key, dims, jnp.float32) * spread
    if len(shards) > 0:
        values = block_scale(key, dims, shards, -0.22, 0.18) * values
    return jnp.clip(values, min=-limit, max=limit).astype(kind)


def setup_inputs(seed: int = 0) -> dict:
    splits = jax.random.split(jax.random.key(seed), 6)
    tokens = gaussian(splits[0], (TOKENS, D), 1.0, 6.0, ((0, 16),))
    norm_gain = jnp.clip(1.0 + 0.18 * jax.random.normal(splits[1], (D,), jnp.float32), 0.1, 1.9)
    gate_weight = gaussian(splits[2], (D, FF), D ** -0.5, 0.125, ((0, 16), (1, 8)))
    up_weight = gaussian(splits[3], (D, FF), D ** -0.5, 0.125, ((0, 16), (1, 8)))
    down_weight = gaussian(splits[4], (FF, D), FF ** -0.5, 0.078125, ((0, 8), (1, 16)))
    return {"tokens": tokens, "norm_gain": norm_gain, "gate_weight": gate_weight, "up_weight": up_weight, "down_weight": down_weight}


def block_rows(xrows, norm_gain, gate_weight, up_weight, down_weight):
    xf = xrows.astype(jnp.float32)
    scale = lax.rsqrt(lax.optimization_barrier(jnp.mean(xf * xf, axis=-1, keepdims=True)) + 1e-06)
    normed = (xf * scale * norm_gain).astype(jnp.bfloat16)
    gate = jnp.dot(normed, gate_weight, preferred_element_type=jnp.float32)
    up = jnp.dot(normed, up_weight, preferred_element_type=jnp.float32)
    hidden = (jax.nn.silu(gate) * up).astype(jnp.bfloat16)
    width = FF // N_TP

    def add_block(total, index):
        start = (index * width).astype(jnp.int32)
        left = lax.dynamic_slice_in_dim(hidden, start, width, 1)
        right = lax.dynamic_slice_in_dim(down_weight, start, width, 0)
        part = jnp.dot(left, right, preferred_element_type=jnp.float32).astype(jnp.bfloat16)
        return (total + part.astype(jnp.float32), None)
    total, unused = lax.scan(add_block, jnp.zeros((xrows.shape[0], D), jnp.float32), jnp.arange(N_TP, dtype=jnp.int32))
    return total.astype(jnp.bfloat16)

def reference(tokens, norm_gain, gate_weight, up_weight, down_weight):
    blocks = tokens.reshape(N_FS, TOKENS // N_FS, D)
    result = lax.map(lambda rows: block_rows(rows, norm_gain, gate_weight, up_weight, down_weight), blocks)
    return result.reshape(TOKENS, D)
```

```python
import functools

import jax
import jax.numpy as jnp
from jax import lax
from jax.experimental import pallas as pl
from jax.experimental.pallas import tpu as pltpu
from jax.sharding import Mesh, PartitionSpec as P


D = 2048
LANES = 128
BLOCKS = 16
WIDTH = 704
ROWS = 256
CHUNKS = 2
PART = ROWS // CHUNKS
VMEM = pl.BlockSpec(memory_space=pltpu.VMEM)
SMEM = pl.BlockSpec(memory_space=pltpu.SMEM)


def masks(core):
    return (1, 3) if core == 0 else (3, 1)


def pair_up(value, axis, step):
    pairs = [(i * 2 + c, (i ^ masks(c)[step]) * 2 + c) for i in range(4) for c in range(2)]
    return lax.ppermute(value, (axis, "c"), pairs)


def double(block, axes):
    have = block[None]
    for axis in axes:
        for step in range(2):
            other = pair_up(have, axis, step)
            if axis == axes[1] and step == 1:
                return have, other
            have = jnp.concatenate([have, other], axis=0)


def swap_order(k):
    return (k >> 2) | ((k & 3) << 2)


def other_core(k):
    return ((k & 1) << 1) | ((k & 2) >> 1) | ((k & 4) << 1) | ((k & 8) >> 1)


def norm_kernel(cols, rows, x_ref, gain_ref, out_ref):
    xf = x_ref[...].astype(jnp.float32)
    scale = lax.rsqrt(jnp.mean(xf * xf, axis=-1, keepdims=True) + 1e-06)
    for k in range(BLOCKS):
        at = pl.multiple_of(cols[k] * LANES, LANES)
        part = x_ref[:, pl.ds(at, LANES)].astype(jnp.float32)
        out_ref[:, k * LANES:(k + 1) * LANES] = (part * scale * gain_ref[:, pl.ds(at, LANES)]).astype(jnp.bfloat16)


def normalize(tokens, gain, cols, rows):
    return pl.pallas_call(
        norm_kernel,
        out_shape=jax.ShapeDtypeStruct(tokens.shape, jnp.bfloat16),
        grid_spec=pltpu.PrefetchScalarGridSpec(
            num_scalar_prefetch=2,
            grid=(tokens.shape[0] // PART,),
            in_specs=[
                pl.BlockSpec((PART, D), lambda i, cols, rows: (rows[i], 0)),
                pl.BlockSpec((1, D), lambda i, cols, rows: (0, 0)),
            ],
            out_specs=pl.BlockSpec((PART, D), lambda i, cols, rows: (i, 0)),
        ),
        name="norm",
    )(cols, rows, tokens, gain.reshape(1, D))


def nt(left, right):
    return lax.dot_general(left, right, (((1,), (1,)), ((), ())), preferred_element_type=jnp.float32)


def hidden_kernel(x_ref, g0, g1, u0, u1, out_ref, gw, uw):
    @pl.when(pl.program_id(0) == 0)
    def _():
        for k in range(BLOCKS):
            gw[:, k * LANES:(k + 1) * LANES] = (g0 if k < 8 else g1)[k % 8]
            s = swap_order(k)
            uw[:, k * LANES:(k + 1) * LANES] = (u0 if s < 8 else u1)[s % 8]

    x = x_ref[...]
    gate = nt(x, gw[...])
    up = nt(x, uw[...])
    out_ref[...] = (gate / (1.0 + jnp.exp(-gate)) * up).astype(jnp.bfloat16)


def hidden_of(normed, gate, up):
    tile = 256
    whole = pl.BlockSpec((8, WIDTH, LANES), lambda i: (0, 0, 0))
    return pl.pallas_call(
        hidden_kernel,
        out_shape=jax.ShapeDtypeStruct((normed.shape[0], WIDTH), jnp.bfloat16),
        grid=(normed.shape[0] // tile,),
        in_specs=[pl.BlockSpec((tile, D), lambda i: (i, 0)), VMEM, VMEM, VMEM, VMEM],
        out_specs=pl.BlockSpec((tile, WIDTH), lambda i: (i, 0)),
        scratch_shapes=[pltpu.VMEM((WIDTH, D), jnp.bfloat16)] * 2,
        compiler_params=pltpu.CompilerParams(vmem_limit_bytes=50 << 20),
        name="hidden",
    )(normed, *gate, *up)


def down_kernel(at, first, last, *refs):
    if last:
        cols, refs = refs[0], refs[1:]
    h_ref, a0, a1, b0, b1 = refs[:5]
    more, out_ref = refs[5:-1], refs[-1]
    h = h_ref[...]
    for k in range(0, BLOCKS, 2):
        w = []
        for j in (k, k + 1):
            j = other_core(j) if first else j
            s = swap_order(j)
            w.append(jnp.concatenate([(a0 if j < 8 else a1)[j % 8], (b0 if s < 8 else b1)[s % 8]], axis=0))
        part = jnp.dot(h, jnp.concatenate(w, axis=1), preferred_element_type=jnp.float32)
        for ref, start in zip(more, at):
            part = part + ref[start:start + h.shape[0], k * LANES:(k + 2) * LANES].astype(jnp.float32)
        part = part.astype(jnp.bfloat16)
        if last:
            for j in range(2):
                out_ref[:, pl.ds(pl.multiple_of(cols[k + j] * LANES, LANES), LANES)] = part[:, j * LANES:(j + 1) * LANES]
        else:
            out_ref[:, k * LANES:(k + 2) * LANES] = part


def down_of(hidden, start, rows, weights, more, name, cols=None):
    last = cols is not None
    return pl.pallas_call(
        functools.partial(down_kernel, [m[1] for m in more], not more, last),
        out_shape=jax.ShapeDtypeStruct((rows, D), jnp.bfloat16),
        grid=(1,),
        in_specs=[SMEM] * last + [pl.BlockSpec((rows, WIDTH), lambda i: (start // rows, 0))] + [VMEM] * (4 + len(more)),
        out_specs=VMEM,
        compiler_params=pltpu.CompilerParams(vmem_limit_bytes=50 << 20),
        name=name,
    )(*([cols] if last else []), hidden, *weights, *[m[0] for m in more])


def per_device(tokens, norm_gain, gate_weight, up_weight, down_weight):
    z, y, x, c = (lax.axis_index(a) for a in "zyxc")
    m1 = jnp.where(c == 0, 1, 3).astype(jnp.int32)
    m2 = 4 - m1
    k = jnp.arange(BLOCKS, dtype=jnp.int32)
    zs = z ^ ((k & 1) * m1) ^ (((k >> 1) & 1) * m2)
    ys = y ^ (((k >> 2) & 1) * m1) ^ (((k >> 3) & 1) * m2)
    cols = zs * 4 + ys
    theirs = jnp.stack([x ^ m1 ^ m2, x ^ m2, x ^ m1, x]) * 2 + (1 - c)
    ours = jnp.stack([x ^ m1 ^ m2, x ^ m1, x ^ m2, x]) * 2 + c
    order = jnp.concatenate([theirs, ours]).astype(jnp.int32)
    rows = (order[None, :] * CHUNKS + jnp.arange(CHUNKS, dtype=jnp.int32)[:, None]).reshape(-1)

    gate = double(gate_weight.T, "zy")
    up = double(up_weight.T, "yz")
    half = WIDTH // 2
    weights = (*double(down_weight[:half], "zy"), *double(down_weight[half:], "yz"))

    normed = normalize(tokens, norm_gain, cols, rows)
    hidden = hidden_of(normed, gate, up)

    outs = []
    for n in range(CHUNKS):
        base = n * 8 * PART
        sent = down_of(hidden, base, 4 * PART, weights, [], f"theirs{n}")
        got = lax.ppermute(sent, "c", [(0, 1), (1, 0)])
        sent = down_of(hidden, base + 4 * PART, 2 * PART, weights, [(got, 0)], f"first{n}")
        got1 = pair_up(sent, "x", 0)
        sent = down_of(hidden, base + 6 * PART, PART, weights, [(got, 2 * PART), (got1, 0)], f"second{n}")
        got2 = pair_up(sent, "x", 1)
        outs.append(down_of(hidden, base + 7 * PART, PART, weights, [(got, 3 * PART), (got1, PART), (got2, 0)], f"last{n}", cols))
    return jnp.concatenate(outs, axis=0)


def solution(mesh):
    torus = Mesh(mesh.devices.reshape(4, 4, 4, 2), ("z", "y", "x", "c"))
    fs, tp = ("z", "y"), ("x", "c")
    placed = (P(fs, None), P(), P(fs, tp), P(fs, tp), P(tp, fs))
    return jax.shard_map(per_device, mesh=torus, in_specs=placed, out_specs=P(fs + tp, None), check_vma=False)
```

```python
import functools

import jax
import jax.numpy as jnp
from jax import lax
from jax.experimental import pallas as pl
from jax.experimental.pallas import tpu as pltpu
from jax.sharding import Mesh, PartitionSpec as P


D = 2048
LANES = 128
BLOCKS = 16
WIDTH = 704
ROWS = 256
CHUNKS = 4
PART = ROWS // CHUNKS
VMEM = pl.BlockSpec(memory_space=pltpu.VMEM)
SMEM = pl.BlockSpec(memory_space=pltpu.SMEM)
ANY = pl.BlockSpec(memory_space=pl.ANY)


def call(kernel, out, mib, **kw):
    return pl.pallas_call(kernel, out_shape=out, compiler_params=pltpu.CompilerParams(vmem_limit_bytes=mib << 20), **kw)


def masks(core):
    return (1, 3) if core == 0 else (3, 1)


def pair_up(value, axis, step):
    pairs = [(i * 2 + c, (i ^ masks(c)[step]) * 2 + c) for i in range(4) for c in range(2)]
    return lax.ppermute(value, (axis, "c"), pairs)


def double(block, route):
    have = block[None]
    for n, (axis, step) in enumerate(route):
        other = pair_up(have, axis, step)
        if n == 3:
            return have, other
        have = jnp.concatenate([have, other], axis=0)


def places(route, z, y, m):
    k = jnp.arange(BLOCKS, dtype=jnp.int32)
    at = {"z": jnp.full_like(k, z), "y": jnp.full_like(k, y)}
    for n, (axis, step) in enumerate(route):
        at[axis] = at[axis] ^ (((k >> n) & 1) * m[step])
    return at["z"] * 4 + at["y"]


ZZYY = (("z", 0), ("z", 1), ("y", 0), ("y", 1))
YYZZ = (("y", 0), ("y", 1), ("z", 0), ("z", 1))
ZYZY = (("z", 0), ("y", 0), ("z", 1), ("y", 1))
YZYZ = (("y", 0), ("z", 0), ("y", 1), ("z", 1))


def norm_kernel(rows, x_ref, gain_ref, out_ref):
    xf = x_ref[...].astype(jnp.float32)
    scale = lax.rsqrt(jnp.mean(xf * xf, axis=-1, keepdims=True) + 1e-06)
    out_ref[...] = (xf * scale * gain_ref[...]).astype(jnp.bfloat16)


def normalize(tokens, gain, rows):
    return call(
        norm_kernel, jax.ShapeDtypeStruct((2 * ROWS, D), jnp.bfloat16), 8,
        grid_spec=pltpu.PrefetchScalarGridSpec(
            num_scalar_prefetch=1,
            grid=(2,),
            in_specs=[pl.BlockSpec((ROWS, D), lambda i, rows: (rows[i], 0)), pl.BlockSpec((1, D), lambda i, rows: (0, 0))],
            out_specs=pl.BlockSpec((ROWS, D), lambda i, rows: (i, 0)),
        ),
    )(rows, tokens, gain.reshape(1, D))


def place_kernel(first, parts, *refs):
    cols, refs = refs[:parts], refs[parts:]
    ins, out_ref = refs[:parts], refs[-1]
    height = WIDTH // parts
    for n in range(parts):
        for k in range(8):
            at = pl.multiple_of(cols[n][first + k] * LANES, LANES)
            out_ref[n * height:(n + 1) * height, pl.ds(at, LANES)] = ins[n][k]


def place(cols, halves, first, into):
    parts = len(halves)
    shape = jax.ShapeDtypeStruct((WIDTH, D), jnp.bfloat16)
    more = [] if into is None else [into]
    return call(
        functools.partial(place_kernel, first, parts), shape, 8,
        in_specs=[SMEM] * parts + [VMEM] * (parts + len(more)), out_specs=VMEM,
        input_output_aliases={2 * parts: 0} if more else {},
    )(*cols, *halves, *more)


def nt(left, right):
    return lax.dot_general(left, right, (((1,), (1,)), ((), ())), preferred_element_type=jnp.float32)


def hidden_kernel(x_ref, gate_ref, up_ref, out_ref):
    x = x_ref[...]
    gate = nt(x, gate_ref[...])
    up = nt(x, up_ref[...])
    hidden = (gate / (1.0 + jnp.exp(-gate)) * up).astype(jnp.bfloat16)
    out_ref[...] = hidden.reshape(out_ref.shape)


def hidden_of(normed, gate, up):
    shape = jax.ShapeDtypeStruct((2, ROWS, WIDTH), jnp.bfloat16)
    return call(hidden_kernel, shape, 20, in_specs=[VMEM] * 3, out_specs=VMEM)(normed, gate, up)


def down_kernel(chunk, picks, n_hidden, at, *refs):
    hidden, down_ref, more, out_ref = refs[:n_hidden], refs[n_hidden], refs[n_hidden + 1:n_hidden + 1 + len(at)], refs[-1]
    rows = slice(chunk * PART, (chunk + 1) * PART)
    h = jnp.concatenate([hidden[i][j, rows, :] for i, j in picks], axis=0)
    for n in range(0, D, 512):
        part = jnp.dot(h, down_ref[:, n:n + 512], preferred_element_type=jnp.float32)
        for ref, start in zip(more, at):
            part = part + ref[start * PART:start * PART + h.shape[0], n:n + 512].astype(jnp.float32)
        out_ref[:, n:n + 512] = part.astype(jnp.bfloat16)


def down_of(chunk, hidden, picks, down, more, into=None):
    rows = len(picks) * PART
    kernel = functools.partial(down_kernel, chunk, picks, len(hidden), [m[1] for m in more])
    ins = [*hidden, down, *[m[0] for m in more]]
    specs = [VMEM] * len(ins)
    if into is None:
        return call(kernel, jax.ShapeDtypeStruct((rows, D), jnp.bfloat16), 12, in_specs=specs, out_specs=VMEM)(*ins)
    first = into is False
    return call(
        kernel, jax.ShapeDtypeStruct((ROWS, D), jnp.bfloat16), 12, grid=(1,),
        in_specs=specs + [] if first else specs + [ANY], out_specs=pl.BlockSpec((rows, D), lambda i: (chunk, 0)),
        input_output_aliases={} if first else {len(ins): 0},
    )(*ins, *([] if first else [into]))


def per_device(tokens, norm_gain, gate_weight, up_weight, down_weight):
    z, y, x, c = (lax.axis_index(a) for a in "zyxc")
    m1 = jnp.where(c == 0, 1, 3).astype(jnp.int32)
    m2 = 4 - m1
    m = (m1, m2)
    theirs = jnp.stack([x ^ m1 ^ m2, x ^ m2, x ^ m1, x]) * 2 + (1 - c)
    ours = jnp.stack([x ^ m1 ^ m2, x ^ m1, x ^ m2, x]) * 2 + c
    order = jnp.concatenate([theirs, ours]).astype(jnp.int32)

    gate = double(gate_weight.T, ZZYY)
    up = double(up_weight.T, YYZZ)
    half = WIDTH // 2
    down = [double(down_weight[:half], ZYZY), double(down_weight[half:], YZYZ)]

    gc, uc = places(ZZYY, z, y, m), places(YYZZ, z, y, m)
    dc = [places(ZYZY, z, y, m), places(YZYZ, z, y, m)]
    normed = [normalize(tokens, norm_gain, order[2 * i:2 * i + 2]) for i in range(4)]
    gw = place([gc], gate[:1], 0, None)
    gw = place([gc], gate[1:], 8, gw)
    uw = place([uc], up[:1], 0, None)
    uw = place([uc], up[1:], 8, uw)
    dw = place(dc, [d[0] for d in down], 0, None)
    dw = place(dc, [d[1] for d in down], 8, dw)
    hid = [hidden_of(normed[i], gw, uw) for i in range(4)]

    out = False
    for n in range(CHUNKS):
        sent = down_of(n, hid[:2], [(0, 0), (0, 1), (1, 0), (1, 1)], dw, [])
        got = lax.ppermute(sent, "c", [(0, 1), (1, 0)])
        sent = down_of(n, hid[2:3], [(0, 0), (0, 1)], dw, [(got, 0)])
        got1 = pair_up(sent, "x", 0)
        sent = down_of(n, hid[3:], [(0, 0)], dw, [(got, 2), (got1, 0)])
        got2 = pair_up(sent, "x", 1)
        out = down_of(n, hid[3:], [(0, 1)], dw, [(got, 3), (got1, 1), (got2, 0)], out)
    return out


def solution(mesh):
    torus = Mesh(mesh.devices.reshape(4, 4, 4, 2), ("z", "y", "x", "c"))
    fs, tp = ("z", "y"), ("x", "c")
    placed = (P(fs, None), P(), P(fs, tp), P(fs, tp), P(tp, fs))
    return jax.shard_map(per_device, mesh=torus, in_specs=placed, out_specs=P(fs + tp, None), check_vma=False)
```

```python
import functools

import jax
import jax.numpy as jnp
from jax import lax
from jax.experimental import pallas as pl
from jax.experimental.pallas import tpu as pltpu
from jax.sharding import Mesh, PartitionSpec as P


D = 2048
LANES = 128
WIDTH = 704
ROWS = 256
CHUNKS = ((0, 48), (48, 112), (160, 64), (224, 32))
VMEM = pl.BlockSpec(memory_space=pltpu.VMEM)
SMEM = pl.BlockSpec(memory_space=pltpu.SMEM)
ANY = pl.BlockSpec(memory_space=pl.ANY)


def call(kernel, out, mib, **kw):
    return pl.pallas_call(kernel, out_shape=out, compiler_params=pltpu.CompilerParams(vmem_limit_bytes=mib << 20), **kw)


def masks(core):
    return (1, 3) if core == 0 else (3, 1)


def pair_up(value, axis, step):
    pairs = [(i * 2 + c, (i ^ masks(c)[step]) * 2 + c) for i in range(4) for c in range(2)]
    return lax.ppermute(value, (axis, "c"), pairs)


def double(block, route):
    have = block[None]
    for n, (axis, step) in enumerate(route):
        other = pair_up(have, axis, step)
        if n == 3:
            return have, other
        have = jnp.concatenate([have, other], axis=0)


def place_of(route, k, pos):
    at = {"z": pos[0], "y": pos[1]}
    m = (1 + 2 * pos[3], 3 - 2 * pos[3])
    for n, (axis, step) in enumerate(route):
        if (k >> n) & 1:
            at[axis] = at[axis] ^ m[step]
    return at["z"] * 4 + at["y"]


def token_block(p, pos):
    core = jnp.where(p < 4, 1 - pos[3], pos[3])
    q = p & 3
    mask = jnp.where(q == 0, 2, jnp.where(q == 1, 1 + 2 * core, jnp.where(q == 2, 3 - 2 * core, 0)))
    return (pos[2] ^ mask) * 2 + core


ZZYY = (("z", 0), ("z", 1), ("y", 0), ("y", 1))
YYZZ = (("y", 0), ("y", 1), ("z", 0), ("z", 1))
ZYZY = (("z", 0), ("y", 0), ("z", 1), ("y", 1))
YZYZ = (("y", 0), ("z", 0), ("y", 1), ("z", 1))


def scale_kernel(x_ref, out_ref):
    for i in range(0, x_ref.shape[0], ROWS):
        xf = x_ref[i:i + ROWS].astype(jnp.float32)
        scale = lax.rsqrt(jnp.mean(xf * xf, axis=-1, keepdims=True) + 1e-06)
        out_ref[i:i + ROWS] = jnp.broadcast_to(scale, (ROWS, LANES))


def scales(tokens):
    return call(
        scale_kernel, jax.ShapeDtypeStruct((tokens.shape[0], LANES), jnp.float32), 12,
        in_specs=[VMEM], out_specs=VMEM,
    )(tokens)


def place_kernel(first, routes, pos, *refs):
    out_ref = refs[-1]
    height = WIDTH // len(routes)
    for n, route in enumerate(routes):
        for k in range(8):
            at = pl.multiple_of(place_of(route, first + k, pos) * LANES, LANES)
            out_ref[n * height:(n + 1) * height, pl.ds(at, LANES)] = refs[n][k]


def place(pos, routes, halves, first, into):
    shape = jax.ShapeDtypeStruct((WIDTH, D), jnp.bfloat16)
    more = [] if into is None else [into]
    return call(
        functools.partial(place_kernel, first, routes), shape, 8,
        in_specs=[SMEM] + [VMEM] * (len(halves) + len(more)), out_specs=VMEM,
        input_output_aliases={1 + len(halves): 0} if more else {},
    )(pos, *halves, *more)


def nt(left, right):
    return lax.dot_general(left, right, (((1,), (1,)), ((), ())), preferred_element_type=jnp.float32)


def hidden_kernel(skip, pos, xa_ref, xb_ref, gate_ref, up_ref, scale_ref, out_ref):
    at = pl.program_id(0) * 2 + skip
    x = jnp.concatenate([xa_ref[...], xb_ref[...]], axis=0)
    rows = [pl.ds(pl.multiple_of(token_block(at + i, pos) * ROWS, ROWS), ROWS) for i in range(2)]
    scale = jnp.concatenate([scale_ref[r, :] for r in rows], axis=0)[:, :1]
    gate = nt(x, gate_ref[...]) * scale
    up = nt(x, up_ref[...]) * scale
    hidden = (gate / (1.0 + jnp.exp(-gate)) * up).astype(jnp.bfloat16)
    out_ref[...] = hidden.reshape(out_ref.shape)


def hidden_of(pos, skip, count, tokens, gate, up, scale):
    return call(
        functools.partial(hidden_kernel, skip), jax.ShapeDtypeStruct((count, ROWS, WIDTH), jnp.bfloat16), 20,
        grid_spec=pltpu.PrefetchScalarGridSpec(
            num_scalar_prefetch=1,
            grid=(count // 2,),
            in_specs=[
                pl.BlockSpec((ROWS, D), lambda i, pos: (token_block(2 * i + skip, pos), 0)),
                pl.BlockSpec((ROWS, D), lambda i, pos: (token_block(2 * i + skip + 1, pos), 0)),
                VMEM, VMEM, VMEM,
            ],
            out_specs=pl.BlockSpec((2, ROWS, WIDTH), lambda i, pos: (i, 0, 0)),
        ),
    )(pos, tokens, tokens, gate, up, scale)


def down_kernel(rows, picks, at, split, *refs):
    n_hidden = max(i for i, _ in picks) + 1
    hidden, down_ref, refs = refs[:n_hidden], refs[n_hidden], refs[n_hidden + 1:]
    more, outs = refs[:len(at)], refs[len(at):]
    size = rows.stop - rows.start
    h = jnp.concatenate([hidden[i][j, rows, :] for i, j in picks], axis=0)
    for n in range(0, D, 512):
        part = jnp.dot(h, down_ref[:, n:n + 512], preferred_element_type=jnp.float32)
        for ref, start in zip(more, at):
            part = part + ref[start * size:start * size + h.shape[0], n:n + 512].astype(jnp.float32)
        outs[0][:, n:n + 512] = (part[:size] if split else part).astype(jnp.bfloat16)
        if split:
            outs[1][:, n:n + 512] = part[size:]


def down_of(chunk, hidden, picks, down, more, split=False):
    start, size = chunk
    kernel = functools.partial(down_kernel, slice(start, start + size), picks, [m[1] for m in more], split)
    ins = [*hidden, down, *[m[0] for m in more]]
    if split:
        out = [jax.ShapeDtypeStruct((size, D), t) for t in (jnp.bfloat16, jnp.float32)]
    else:
        out = jax.ShapeDtypeStruct((len(picks) * size, D), jnp.bfloat16)
    return call(kernel, out, 12, in_specs=[VMEM] * len(ins), out_specs=[VMEM] * 2 if split else VMEM)(*ins)


def last_kernel(rows, own_ref, got_ref, *refs):
    out_ref, buf, sem = refs[-3:]
    buf[...] = (own_ref[...] + got_ref[...].astype(jnp.float32)).astype(jnp.bfloat16)
    copy = pltpu.make_async_copy(buf, out_ref.at[rows], sem)
    copy.start()
    copy.wait()


def last_of(chunk, own, got, into):
    start, size = chunk
    more = [] if into is None else [into]
    return call(
        functools.partial(last_kernel, slice(start, start + size)), jax.ShapeDtypeStruct((ROWS, D), jnp.bfloat16), 8,
        in_specs=[VMEM] * 2 + [ANY] * len(more), out_specs=ANY,
        scratch_shapes=[pltpu.VMEM((size, D), jnp.bfloat16), pltpu.SemaphoreType.DMA],
        input_output_aliases={2: 0} if more else {},
    )(own, got, *more)


def per_device(tokens, norm_gain, gate_weight, up_weight, down_weight):
    z, y, x, c = (lax.axis_index(a) for a in "zyxc")
    k = jnp.arange(4, dtype=jnp.int32)
    pos = jnp.where(k == 0, z, jnp.where(k == 1, y, jnp.where(k == 2, x, c)))
    half = WIDTH // 2
    blocks = [gate_weight.T, up_weight.T, down_weight[:half], down_weight[half:]]
    gain = lax.dynamic_slice(norm_gain, ((z * 4 + y) * LANES,), (LANES,))
    for i in range(2):
        blocks[i] = (blocks[i].astype(jnp.float32) * gain).astype(jnp.bfloat16)
    blocks[0], blocks[1], pos = lax.optimization_barrier((blocks[0], blocks[1], pos))
    gate = double(blocks[0], ZZYY)
    up = double(blocks[1], YYZZ)
    down = [double(blocks[2], ZYZY), double(blocks[3], YZYZ)]

    scale = scales(tokens)
    gw = place(pos, [ZZYY], gate[:1], 0, None)
    gw = place(pos, [ZZYY], gate[1:], 8, gw)
    uw = place(pos, [YYZZ], up[:1], 0, None)
    uw = place(pos, [YYZZ], up[1:], 8, uw)
    hid = [hidden_of(pos, n, m, tokens, gw, uw, scale) for n, m in ((0, 2), (2, 6))]
    dw = place(pos, [ZYZY, YZYZ], [d[0] for d in down], 0, None)
    dw = place(pos, [ZYZY, YZYZ], [d[1] for d in down], 8, dw)

    out = None
    for chunk in CHUNKS:
        sent = down_of(chunk, hid, [(0, 0), (0, 1), (1, 0), (1, 1)], dw, [])
        got = lax.ppermute(sent, "c", [(0, 1), (1, 0)])
        sent = down_of(chunk, hid[1:], [(0, 2), (0, 3)], dw, [(got, 0)])
        got1 = pair_up(sent, "x", 0)
        sent, own = down_of(chunk, hid[1:], [(0, 4), (0, 5)], dw, [(got, 2), (got1, 0)], True)
        got2 = pair_up(sent, "x", 1)
        out = last_of(chunk, own, got2, out)
    return out


def solution(mesh):
    torus = Mesh(mesh.devices.reshape(4, 4, 4, 2), ("z", "y", "x", "c"))
    fs, tp = ("z", "y"), ("x", "c")
    placed = (P(fs, None), P(), P(fs, tp), P(fs, tp), P(tp, fs))
    return jax.shard_map(per_device, mesh=torus, in_specs=placed, out_specs=P(fs + tp, None), check_vma=False)
```

```python
import functools

import jax
import jax.numpy as jnp
from jax import lax
from jax.experimental import pallas as pl
from jax.experimental.pallas import tpu as pltpu
from jax.sharding import Mesh, PartitionSpec as P


D = 2048
LANES = 128
WIDTH = 704
ROWS = 256
CHUNKS = ((0, 48), (48, 144), (192, 64))
VMEM = pl.BlockSpec(memory_space=pltpu.VMEM)
SMEM = pl.BlockSpec(memory_space=pltpu.SMEM)
ANY = pl.BlockSpec(memory_space=pl.ANY)


def call(kernel, out, mib, **kw):
    return pl.pallas_call(kernel, out_shape=out, compiler_params=pltpu.CompilerParams(vmem_limit_bytes=mib << 20), **kw)


def masks(core):
    return (1, 3) if core == 0 else (3, 1)


def pair_up(value, axis, step):
    pairs = [(i * 2 + c, (i ^ masks(c)[step]) * 2 + c) for i in range(4) for c in range(2)]
    return lax.ppermute(value, (axis, "c"), pairs)


def double(have, route, steps=range(4)):
    for n in steps:
        axis, step = route[n]
        other = pair_up(have, axis, step)
        if n == 3:
            return have, other
        have = jnp.concatenate([have, other], axis=0)
    return have


def place_of(route, k, pos):
    at = {"z": pos[0], "y": pos[1]}
    m = (1 + 2 * pos[3], 3 - 2 * pos[3])
    for n, (axis, step) in enumerate(route):
        if (k >> n) & 1:
            at[axis] = at[axis] ^ m[step]
    return at["z"] * 4 + at["y"]


def token_block(p, pos):
    core = jnp.where(p < 4, 1 - pos[3], pos[3])
    q = p & 3
    mask = jnp.where(q == 0, 2, jnp.where(q == 1, 1 + 2 * core, jnp.where(q == 2, 3 - 2 * core, 0)))
    return (pos[2] ^ mask) * 2 + core


ZZYY = (("z", 0), ("z", 1), ("y", 0), ("y", 1))
YYZZ = (("y", 0), ("y", 1), ("z", 0), ("z", 1))
ZYZY = (("z", 0), ("y", 0), ("z", 1), ("y", 1))
ZYYZ = (("z", 0), ("y", 0), ("y", 1), ("z", 1))


def scale_kernel(x_ref, out_ref):
    for i in range(0, x_ref.shape[0], ROWS):
        xf = x_ref[i:i + ROWS].astype(jnp.float32)
        scale = lax.rsqrt(jnp.mean(xf * xf, axis=-1, keepdims=True) + 1e-06)
        out_ref[i:i + ROWS] = jnp.broadcast_to(scale, (ROWS, LANES))


def scales(tokens):
    return call(
        scale_kernel, jax.ShapeDtypeStruct((tokens.shape[0], LANES), jnp.float32), 12,
        in_specs=[VMEM], out_specs=VMEM,
    )(tokens)


def place_kernel(first, routes, pos, *refs):
    out_ref = refs[-1]
    height = WIDTH // len(routes)
    for n, route in enumerate(routes):
        for k in range(8):
            at = pl.multiple_of(place_of(route, first + k, pos) * LANES, LANES)
            out_ref[n * height:(n + 1) * height, pl.ds(at, LANES)] = refs[n][k]


def place(pos, routes, halves, first, into):
    shape = jax.ShapeDtypeStruct((WIDTH, D), jnp.bfloat16)
    more = [] if into is None else [into]
    return call(
        functools.partial(place_kernel, first, routes), shape, 8,
        in_specs=[SMEM] + [VMEM] * (len(halves) + len(more)), out_specs=VMEM,
        input_output_aliases={1 + len(halves): 0} if more else {},
    )(pos, *halves, *more)


def nt(left, right):
    return lax.dot_general(left, right, (((1,), (1,)), ((), ())), preferred_element_type=jnp.float32)


def stack_kernel(g_ref, u_ref, gw_ref, uw_ref):
    for k in range(8):
        gw_ref[:, k * LANES:(k + 1) * LANES] = g_ref[k]
        uw_ref[:, k * LANES:(k + 1) * LANES] = u_ref[k]


def stack(gate, up):
    return call(
        stack_kernel, [jax.ShapeDtypeStruct((WIDTH, D // 2), jnp.bfloat16)] * 2, 8,
        in_specs=[VMEM] * 2, out_specs=[VMEM] * 2,
    )(gate, up)


def hidden_kernel(skip, half, pos, xa_ref, xb_ref, gate_ref, up_ref, *refs):
    gx, ux = refs[-2:]
    for route, xs in ((ZZYY, gx), (YYZZ, ux)):
        for k in range(8):
            at = pl.multiple_of(place_of(route, 8 * half + k, pos) * LANES, LANES)
            xs[:ROWS, k * LANES:(k + 1) * LANES] = xa_ref[:, pl.ds(at, LANES)]
            xs[ROWS:, k * LANES:(k + 1) * LANES] = xb_ref[:, pl.ds(at, LANES)]
    gate = nt(gx[...], gate_ref[...])
    up = nt(ux[...], up_ref[...])
    if half == 0:
        refs[0][...] = gate
        refs[1][...] = up
        return
    at = pl.program_id(0) * 2 + skip
    rows = [pl.ds(pl.multiple_of(token_block(at + i, pos) * ROWS, ROWS), ROWS) for i in range(2)]
    scale = jnp.concatenate([refs[2][r, :] for r in rows], axis=0)[:, :1]
    gate = (gate + refs[0][...]) * scale
    up = (up + refs[1][...]) * scale
    hidden = (gate / (1.0 + jnp.exp(-gate)) * up).astype(jnp.bfloat16)
    refs[3][...] = hidden.reshape(refs[3].shape)


def hidden_of(pos, half, skip, count, tokens, weights, more):
    tile = 2 * ROWS
    sums = pl.BlockSpec((tile, WIDTH), lambda i, pos: (i + skip // 2, 0))
    if half:
        out = jax.ShapeDtypeStruct((count, ROWS, WIDTH), jnp.bfloat16)
        out_specs = pl.BlockSpec((2, ROWS, WIDTH), lambda i, pos: (i, 0, 0))
    else:
        out = [jax.ShapeDtypeStruct((count * ROWS, WIDTH), jnp.float32)] * 2
        out_specs = [sums] * 2
    return call(
        functools.partial(hidden_kernel, skip, half), out, 16,
        grid_spec=pltpu.PrefetchScalarGridSpec(
            num_scalar_prefetch=1,
            grid=(count // 2,),
            in_specs=[
                pl.BlockSpec((ROWS, D), lambda i, pos: (token_block(2 * i + skip, pos), 0)),
                pl.BlockSpec((ROWS, D), lambda i, pos: (token_block(2 * i + skip + 1, pos), 0)),
                VMEM, VMEM,
            ] + ([sums, sums, VMEM] if half else []),
            out_specs=out_specs,
            scratch_shapes=[pltpu.VMEM((tile, D // 2), jnp.bfloat16)] * 2,
        ),
    )(pos, tokens, tokens, *weights, *more)


def down_kernel(rows, picks, at, split, *refs):
    n_hidden = max(i for i, _ in picks) + 1
    hidden, down_ref, refs = refs[:n_hidden], refs[n_hidden], refs[n_hidden + 1:]
    more, outs = refs[:len(at)], refs[len(at):]
    size = rows.stop - rows.start
    h = jnp.concatenate([hidden[i][j, rows, :] for i, j in picks], axis=0)
    for n in range(0, D, 512):
        part = jnp.dot(h, down_ref[:, n:n + 512], preferred_element_type=jnp.float32)
        for ref, start in zip(more, at):
            part = part + ref[start * size:start * size + h.shape[0], n:n + 512].astype(jnp.float32)
        outs[0][:, n:n + 512] = (part[:size] if split else part).astype(jnp.bfloat16)
        if split:
            outs[1][:, n:n + 512] = part[size:]


def down_of(chunk, hidden, picks, down, more, split=False):
    start, size = chunk
    kernel = functools.partial(down_kernel, slice(start, start + size), picks, [m[1] for m in more], split)
    ins = [*hidden, down, *[m[0] for m in more]]
    if split:
        out = [jax.ShapeDtypeStruct((size, D), t) for t in (jnp.bfloat16, jnp.float32)]
    else:
        out = jax.ShapeDtypeStruct((len(picks) * size, D), jnp.bfloat16)
    return call(kernel, out, 12, in_specs=[VMEM] * len(ins), out_specs=[VMEM] * 2 if split else VMEM)(*ins)


def last_kernel(rows, own_ref, got_ref, *refs):
    out_ref, buf, sem = refs[-3:]
    buf[...] = (own_ref[...] + got_ref[...].astype(jnp.float32)).astype(jnp.bfloat16)
    copy = pltpu.make_async_copy(buf, out_ref.at[rows], sem)
    copy.start()
    copy.wait()


def last_of(chunk, own, got, into):
    start, size = chunk
    more = [] if into is None else [into]
    return call(
        functools.partial(last_kernel, slice(start, start + size)), jax.ShapeDtypeStruct((ROWS, D), jnp.bfloat16), 8,
        in_specs=[VMEM] * 2 + [ANY] * len(more), out_specs=ANY,
        scratch_shapes=[pltpu.VMEM((size, D), jnp.bfloat16), pltpu.SemaphoreType.DMA],
        input_output_aliases={2: 0} if more else {},
    )(own, got, *more)


def per_device(tokens, norm_gain, gate_weight, up_weight, down_weight):
    z, y, x, c = (lax.axis_index(a) for a in "zyxc")
    k = jnp.arange(4, dtype=jnp.int32)
    pos = jnp.where(k == 0, z, jnp.where(k == 1, y, jnp.where(k == 2, x, c)))
    half = WIDTH // 2
    blocks = [gate_weight.T, up_weight.T]
    gain = lax.dynamic_slice(norm_gain, ((z * 4 + y) * LANES,), (LANES,))
    for i in range(2):
        blocks[i] = (blocks[i].astype(jnp.float32) * gain).astype(jnp.bfloat16)
    blocks[0], blocks[1], pos = lax.optimization_barrier((blocks[0], blocks[1], pos))
    gate = double(blocks[0][None], ZZYY)
    up = double(blocks[1][None], YYZZ)
    down = double(down_weight[None], ZYZY, range(2))
    down = [double(down[:, :half], ZYZY, range(2, 4)), double(down[:, half:], ZYYZ, range(2, 4))]
    scale = scales(tokens)
    partial = hidden_of(pos, 0, 0, 8, tokens, stack(gate[0], up[0]), [])
    rest = stack(gate[1], up[1])
    hid = [hidden_of(pos, 1, n, 4, tokens, rest, [*partial, scale]) for n in (0, 4)]
    dw = place(pos, [ZYZY, ZYYZ], [d[0] for d in down], 0, None)
    dw = place(pos, [ZYZY, ZYYZ], [d[1] for d in down], 8, dw)

    out = None
    for chunk in CHUNKS:
        sent = down_of(chunk, hid[:1], [(0, 0), (0, 1), (0, 2), (0, 3)], dw, [])
        got = lax.ppermute(sent, "c", [(0, 1), (1, 0)])
        sent = down_of(chunk, hid[1:], [(0, 0), (0, 1)], dw, [(got, 0)])
        got1 = pair_up(sent, "x", 0)
        sent, own = down_of(chunk, hid[1:], [(0, 2), (0, 3)], dw, [(got, 2), (got1, 0)], True)
        got2 = pair_up(sent, "x", 1)
        out = last_of(chunk, own, got2, out)
    return out


def solution(mesh):
    torus = Mesh(mesh.devices.reshape(4, 4, 4, 2), ("z", "y", "x", "c"))
    fs, tp = ("z", "y"), ("x", "c")
    placed = (P(fs, None), P(), P(fs, tp), P(fs, tp), P(tp, fs))
    return jax.shard_map(per_device, mesh=torus, in_specs=placed, out_specs=P(fs + tp, None), check_vma=False)
```

```python
import functools

import jax
import jax.numpy as jnp
from jax import lax
from jax.experimental import pallas as pl
from jax.experimental.pallas import tpu as pltpu
from jax.sharding import Mesh, PartitionSpec as P


D = 2048
LANES = 128
WIDTH = 704
ROWS = 256
CHUNKS = ((0, 64), (64, 144), (208, 48))
VMEM = pl.BlockSpec(memory_space=pltpu.VMEM)
SMEM = pl.BlockSpec(memory_space=pltpu.SMEM)
ANY = pl.BlockSpec(memory_space=pl.ANY)


def call(kernel, out, mib, **kw):
    return pl.pallas_call(kernel, out_shape=out, compiler_params=pltpu.CompilerParams(vmem_limit_bytes=mib << 20), **kw)


def masks(core):
    return (1, 3) if core == 0 else (3, 1)


def pair_up(value, axis, step):
    pairs = [(i * 2 + c, (i ^ masks(c)[step]) * 2 + c) for i in range(4) for c in range(2)]
    return lax.ppermute(value, (axis, "c"), pairs)


def double(have, route, steps=range(4)):
    for n in steps:
        axis, step = route[n]
        other = pair_up(have, axis, step)
        if n == 3:
            return have, other
        have = jnp.concatenate([have, other], axis=0)
    return have


def place_of(route, k, pos):
    at = {"z": pos[0], "y": pos[1]}
    m = (1 + 2 * pos[3], 3 - 2 * pos[3])
    for n, (axis, step) in enumerate(route):
        if (k >> n) & 1:
            at[axis] = at[axis] ^ m[step]
    return at["z"] * 4 + at["y"]


def token_block(p, pos):
    core = jnp.where(p < 4, 1 - pos[3], pos[3])
    q = p & 3
    mask = jnp.where(q == 0, 2, jnp.where(q == 1, 1 + 2 * core, jnp.where(q == 2, 3 - 2 * core, 0)))
    return (pos[2] ^ mask) * 2 + core


ZZYY = (("z", 0), ("z", 1), ("y", 0), ("y", 1))
YYZZ = (("y", 0), ("y", 1), ("z", 0), ("z", 1))
ZYZY = (("z", 0), ("y", 0), ("z", 1), ("y", 1))
ZYYZ = (("z", 0), ("y", 0), ("y", 1), ("z", 1))


def scale_kernel(x_ref, out_ref):
    for i in range(0, x_ref.shape[0], ROWS):
        xf = x_ref[i:i + ROWS].astype(jnp.float32)
        scale = lax.rsqrt(jnp.mean(xf * xf, axis=-1, keepdims=True) + 1e-06)
        out_ref[i:i + ROWS] = jnp.broadcast_to(scale, (ROWS, LANES))


def scales(tokens):
    return call(
        scale_kernel, jax.ShapeDtypeStruct((tokens.shape[0], LANES), jnp.float32), 12,
        in_specs=[VMEM], out_specs=VMEM,
    )(tokens)


def place_kernel(first, routes, pos, *refs):
    out_ref = refs[-1]
    height = WIDTH // len(routes)
    for n, route in enumerate(routes):
        for k in range(8):
            at = pl.multiple_of(place_of(route, first + k, pos) * LANES, LANES)
            out_ref[n * height:(n + 1) * height, pl.ds(at, LANES)] = refs[n][k]


def place(pos, routes, halves, first, into):
    shape = jax.ShapeDtypeStruct((WIDTH, D), jnp.bfloat16)
    more = [] if into is None else [into]
    return call(
        functools.partial(place_kernel, first, routes), shape, 8,
        in_specs=[SMEM] + [VMEM] * (len(halves) + len(more)), out_specs=VMEM,
        input_output_aliases={1 + len(halves): 0} if more else {},
    )(pos, *halves, *more)


def nt(left, right):
    return lax.dot_general(left, right, (((1,), (1,)), ((), ())), preferred_element_type=jnp.float32)


def stack_kernel(g_ref, u_ref, gw_ref, uw_ref):
    for k in range(8):
        gw_ref[:, k * LANES:(k + 1) * LANES] = g_ref[k]
        uw_ref[:, k * LANES:(k + 1) * LANES] = u_ref[k]


def stack(gate, up):
    return call(
        stack_kernel, [jax.ShapeDtypeStruct((WIDTH, D // 2), jnp.bfloat16)] * 2, 8,
        in_specs=[VMEM] * 2, out_specs=[VMEM] * 2,
    )(gate, up)


def hidden_kernel(skip, half, pos, xa_ref, xb_ref, gate_ref, up_ref, *refs):
    gx, ux = refs[-2:]
    for route, xs in ((ZZYY, gx), (YYZZ, ux)):
        for k in range(8):
            at = pl.multiple_of(place_of(route, 8 * half + k, pos) * LANES, LANES)
            xs[:ROWS, k * LANES:(k + 1) * LANES] = xa_ref[:, pl.ds(at, LANES)]
            xs[ROWS:, k * LANES:(k + 1) * LANES] = xb_ref[:, pl.ds(at, LANES)]
    gate = nt(gx[...], gate_ref[...])
    up = nt(ux[...], up_ref[...])
    if half == 0:
        refs[0][...] = gate
        refs[1][...] = up
        return
    at = pl.program_id(0) * 2 + skip
    rows = [pl.ds(pl.multiple_of(token_block(at + i, pos) * ROWS, ROWS), ROWS) for i in range(2)]
    scale = jnp.concatenate([refs[2][r, :] for r in rows], axis=0)[:, :1]
    gate = (gate + refs[0][...]) * scale
    up = (up + refs[1][...]) * scale
    hidden = (gate / (1.0 + jnp.exp(-gate)) * up).astype(jnp.bfloat16)
    refs[3][...] = hidden.reshape(refs[3].shape)


def hidden_of(pos, half, skip, count, tokens, weights, more):
    tile = 2 * ROWS
    sums = pl.BlockSpec((tile, WIDTH), lambda i, pos: (i + skip // 2, 0))
    if half:
        out = jax.ShapeDtypeStruct((count, ROWS, WIDTH), jnp.bfloat16)
        out_specs = pl.BlockSpec((2, ROWS, WIDTH), lambda i, pos: (i, 0, 0))
    else:
        out = [jax.ShapeDtypeStruct((count * ROWS, WIDTH), jnp.float32)] * 2
        out_specs = [sums] * 2
    return call(
        functools.partial(hidden_kernel, skip, half), out, 16,
        grid_spec=pltpu.PrefetchScalarGridSpec(
            num_scalar_prefetch=1,
            grid=(count // 2,),
            in_specs=[
                pl.BlockSpec((ROWS, D), lambda i, pos: (token_block(2 * i + skip, pos), 0)),
                pl.BlockSpec((ROWS, D), lambda i, pos: (token_block(2 * i + skip + 1, pos), 0)),
                VMEM, VMEM,
            ] + ([sums, sums, VMEM] if half else []),
            out_specs=out_specs,
            scratch_shapes=[pltpu.VMEM((tile, D // 2), jnp.bfloat16)] * 2,
        ),
    )(pos, tokens, tokens, *weights, *more)


def down_kernel(rows, picks, at, split, *refs):
    n_hidden = max(i for i, _ in picks) + 1
    hidden, down_ref, refs = refs[:n_hidden], refs[n_hidden], refs[n_hidden + 1:]
    more, outs = refs[:len(at)], refs[len(at):]
    size = rows.stop - rows.start
    h = jnp.concatenate([hidden[i][j, rows, :] for i, j in picks], axis=0)
    for n in range(0, D, 512):
        part = jnp.dot(h, down_ref[:, n:n + 512], preferred_element_type=jnp.float32)
        for ref, start in zip(more, at):
            part = part + ref[start * size:start * size + h.shape[0], n:n + 512].astype(jnp.float32)
        outs[0][:, n:n + 512] = (part[:size] if split else part).astype(jnp.bfloat16)
        if split:
            outs[1][:, n:n + 512] = part[size:]


def down_of(chunk, hidden, picks, down, more, split=False):
    start, size = chunk
    kernel = functools.partial(down_kernel, slice(start, start + size), picks, [m[1] for m in more], split)
    ins = [*hidden, down, *[m[0] for m in more]]
    if split:
        out = [jax.ShapeDtypeStruct((size, D), t) for t in (jnp.bfloat16, jnp.float32)]
    else:
        out = jax.ShapeDtypeStruct((len(picks) * size, D), jnp.bfloat16)
    return call(kernel, out, 12, in_specs=[VMEM] * len(ins), out_specs=[VMEM] * 2 if split else VMEM)(*ins)


def last_kernel(rows, own_ref, got_ref, *refs):
    out_ref, buf, sem = refs[-3:]
    buf[...] = (own_ref[...] + got_ref[...].astype(jnp.float32)).astype(jnp.bfloat16)
    copy = pltpu.make_async_copy(buf, out_ref.at[rows], sem)
    copy.start()
    copy.wait()


def last_of(chunk, own, got, into):
    start, size = chunk
    more = [] if into is None else [into]
    return call(
        functools.partial(last_kernel, slice(start, start + size)), jax.ShapeDtypeStruct((ROWS, D), jnp.bfloat16), 8,
        in_specs=[VMEM] * 2 + [ANY] * len(more), out_specs=ANY,
        scratch_shapes=[pltpu.VMEM((size, D), jnp.bfloat16), pltpu.SemaphoreType.DMA],
        input_output_aliases={2: 0} if more else {},
    )(own, got, *more)


def per_device(tokens, norm_gain, gate_weight, up_weight, down_weight):
    z, y, x, c = (lax.axis_index(a) for a in "zyxc")
    k = jnp.arange(4, dtype=jnp.int32)
    pos = jnp.where(k == 0, z, jnp.where(k == 1, y, jnp.where(k == 2, x, c)))
    half = WIDTH // 2
    blocks = [gate_weight.T, up_weight.T]
    gain = lax.dynamic_slice(norm_gain, ((z * 4 + y) * LANES,), (LANES,))
    for i in range(2):
        blocks[i] = (blocks[i].astype(jnp.float32) * gain).astype(jnp.bfloat16)
    blocks[0], blocks[1], pos = lax.optimization_barrier((blocks[0], blocks[1], pos))
    gate = double(blocks[0][None], ZZYY)
    up = double(blocks[1][None], YYZZ)
    down = double(down_weight[None], ZYZY, range(2))
    down = [double(down[:, :half], ZYZY, range(2, 4)), double(down[:, half:], ZYYZ, range(2, 4))]
    scale = scales(tokens)
    partial = hidden_of(pos, 0, 0, 8, tokens, stack(gate[0], up[0]), [])
    rest = stack(gate[1], up[1])
    hid = [hidden_of(pos, 1, n, m, tokens, rest, [*partial, scale]) for n, m in ((0, 4), (4, 2), (6, 2))]
    dw = place(pos, [ZYZY, ZYYZ], [d[0] for d in down], 0, None)
    dw = place(pos, [ZYZY, ZYYZ], [d[1] for d in down], 8, dw)

    out = None
    for chunk in CHUNKS:
        sent = down_of(chunk, hid[:1], [(0, 0), (0, 1), (0, 2), (0, 3)], dw, [])
        got = lax.ppermute(sent, "c", [(0, 1), (1, 0)])
        sent = down_of(chunk, hid[1:2], [(0, 0), (0, 1)], dw, [(got, 0)])
        got1 = pair_up(sent, "x", 0)
        sent, own = down_of(chunk, hid[2:], [(0, 0), (0, 1)], dw, [(got, 2), (got1, 0)], True)
        got2 = pair_up(sent, "x", 1)
        out = last_of(chunk, own, got2, out)
    return out


def solution(mesh):
    torus = Mesh(mesh.devices.reshape(4, 4, 4, 2), ("z", "y", "x", "c"))
    fs, tp = ("z", "y"), ("x", "c")
    placed = (P(fs, None), P(), P(fs, tp), P(fs, tp), P(tp, fs))
    return jax.shard_map(per_device, mesh=torus, in_specs=placed, out_specs=P(fs + tp, None), check_vma=False)
```
